32 devices in a mesh: grp: 2 (over y), fs: 4 (over z), tp: 4 (over x, core).
Axes of the slice: x: 2, y: 2, z: 4, core: 2. Of those that a mesh axis runs over, the one named last changes fastest.
Arguments:
- tokens: bfloat16 [2048, 2048], P(('grp', 'fs')), parts along dimension 0, may hold values from -6 to 6
- decay_logs: float32 [8, 2048], P('tp', ('grp', 'fs')), parts along dimension 1, may hold values from -1.5 to 0, as said below
- query_weight: float32 [2048, 1024], P('fs', 'tp'), may hold values from -0.125 to 0.125
- key_weight: float32 [2048, 1024], P('fs', 'tp'), may hold values from -0.125 to 0.125
- value_weight: float32 [2048, 2048], P('fs', 'tp'), may hold values from -0.125 to 0.125
- out_weight: float32 [2048, 2048], P('tp', 'fs'), may hold values from -0.125 to 0.125
- gate_weight: float32 [2048, 5632], P('fs', 'tp'), may hold values from -0.125 to 0.125
- up_weight: float32 [2048, 5632], P('fs', 'tp'), may hold values from -0.125 to 0.125
- down_weight: float32 [5632, 2048], P('tp', 'fs'), may hold values from -0.078125 to 0.078125
- query_scale: float32 [1024], P(('tp', 'fs')), may hold values from 0.5 to 2
- key_scale: float32 [1024], P(('tp', 'fs')), may hold values from 0.5 to 2
- value_scale: float32 [2048], P(('tp', 'fs')), may hold values from 0.5 to 2
- out_scale: float32 [2048], P('fs'), may hold values from 0.5 to 2
- gate_scale: float32 [5632], P(('tp', 'fs')), may hold values from 0.5 to 2
- up_scale: float32 [5632], P(('tp', 'fs')), may hold values from 0.5 to 2
- down_scale: float32 [2048], P('fs'), may hold values from 0.5 to 2
- conv_weight: float32 [3, 5632], P(None, 'tp'), may hold values from -3.5 to 3.5
- conv_bias: float32 [5632], P('tp'), may hold values from -3 to 3
- first_gain: float32 [2048], replicated, may hold values from 0.1 to 1.9
- first_bias: float32 [2048], replicated, may hold values from -3 to 3
- second_gain: float32 [2048], replicated, may hold values from 0.1 to 1.9
- second_bias: float32 [2048], replicated, may hold values from -3 to 3
Outputs:
- layer_out: bfloat16 [2048, 2048], P(('grp', 'fs', 'tp')), parts along dimension 0
The draws below stay inside these ranges and needn't reach their ends.
There are 2 independent parts, one for each index of `grp`. The reference program is written for one: setup_inputs(seed, part) draws one part's arguments, and reference() takes and returns one part's arrays. A program takes and returns all parts, laid end to end along the dimension named above; an argument that names none is the same for every part. Nothing has to cross between parts.
Inputs may be any that keep to these rules, and one draw needn't show every extreme that they name: `decay_logs`: log-decays are negative; each head's rate is steady along a sequence except at a few positions.
All inputs are finite; a program needn't handle non-finite values.
Results may differ from the reference program's by a relative error of at most 0.018.
Values may be sent and summed in bfloat16 or wider, within the bound.
A program may use at most 64 MiB of HBM per device.

```python
import math
import jax
import jax.numpy as jnp
from jax import lax

D = 2048
RETENTION_HEADS = 8
QK_HEAD = 128
V_HEAD = 256
FF = 5632
SEQUENCE_TOKENS = 256
BLOCK = 128
KERNEL = 3
QK_WIDTH = 1024
V_WIDTH = 2048
TOTAL_TOKENS = 1024
N_TP = 4


def draw_decay_logs(key, part):
    random_subkeys = jax.random.split(jax.random.fold_in(key, 17), 6)
    sequence_list = TOTAL_TOKENS // SEQUENCE_TOKENS
    quick_share = 0.5
    quick_heads = jax.random.uniform(random_subkeys[0], (RETENTION_HEADS, 1, 1)) < quick_share
    quick_rate = 1.0 / jax.random.uniform(random_subkeys[1], (RETENTION_HEADS, 1, 1), minval=30.0, maxval=100.0)
    slow_rate = math.log(10.0) * jax.random.uniform(random_subkeys[2], (RETENTION_HEADS, 1, 1), minval=0.1, maxval=0.3) / SEQUENCE_TOKENS
    factor = jnp.exp(jax.random.uniform(random_subkeys[3], (1, sequence_list, 1), minval=0.0, maxval=math.log(2.5)))
    baseline_level = -jnp.where(quick_heads, quick_rate, slow_rate) * factor
    spike_positions = jax.random.randint(random_subkeys[4], (RETENTION_HEADS, sequence_list, 2, 1), 0, SEQUENCE_TOKENS)
    spike_logarithms = jnp.log(jax.random.uniform(random_subkeys[5], (RETENTION_HEADS, sequence_list, 2, 1), minval=0.5, maxval=0.8))
    spike_present = jnp.arange(SEQUENCE_TOKENS)[None, None, None, :] == spike_positions
    spike_events = jnp.sum(jnp.where(spike_present, spike_logarithms, 0.0), axis=2)
    return (baseline_level + spike_events).reshape(RETENTION_HEADS, TOTAL_TOKENS).astype(jnp.float32)


def block_levels(own_key, shape, shards, smallest, largest):
    level, own = 1.0, jax.random.fold_in(own_key, 6)
    for axis_at, shards_of in shards:
        draws = jnp.exp(jax.random.uniform(jax.random.fold_in(own, axis_at), (shards_of,), jnp.float32, smallest / len(shards), largest / len(shards)))
        level = level * jnp.repeat(draws, shape[axis_at] // shards_of).reshape([-1 if axis == axis_at else 1 for axis in range(len(shape))])
    return level


def normal_values(rng, shape, deviation, most, shards=(), held_as=jnp.bfloat16):
    array = jax.random.normal(rng, shape, jnp.float32) * deviation
    if len(shards) > 0:
        array = block_levels(rng, shape, shards, -0.22, 0.18) * array
    return jnp.clip(array, min=-most, max=most).astype(held_as)


def setup_inputs(seed: int = 0, part: int = 0) -> dict:
    key_of = jax.random.split(jax.random.key(seed), 23)
    part_splits = jax.random.split(jax.random.fold_in(key_of[22], part), 23)
    return {
        "tokens": normal_values(part_splits[0], (TOTAL_TOKENS, D), 1.0, 6.0, ((0, 4),)),
        "decay_logs": draw_decay_logs(jax.random.fold_in(jax.random.fold_in(key_of[22], part), 71), part),
        "query_weight": normal_values(key_of[2], (D, QK_WIDTH), D ** -0.5, 0.125, ((0, 4), (1, 4)), jnp.float32),
        "key_weight": normal_values(key_of[3], (D, QK_WIDTH), D ** -0.5, 0.125, ((0, 4), (1, 4)), jnp.float32),
        "value_weight": normal_values(key_of[4], (D, V_WIDTH), D ** -0.5, 0.125, ((0, 4), (1, 4)), jnp.float32),
        "out_weight": normal_values(key_of[5], (V_WIDTH, D), V_WIDTH ** -0.5, 0.125, ((0, 4), (1, 4)), jnp.float32),
        "gate_weight": normal_values(key_of[6], (D, FF), D ** -0.5, 0.125, ((0, 4), (1, 4)), jnp.float32),
        "up_weight": normal_values(key_of[7], (D, FF), D ** -0.5, 0.125, ((0, 4), (1, 4)), jnp.float32),
        "down_weight": normal_values(key_of[8], (FF, D), FF ** -0.5, 0.078125, ((0, 4), (1, 4)), jnp.float32),
        "query_scale": jnp.clip(jnp.exp(math.log(2.0) - 1.3862944 * jax.random.uniform(key_of[9], (QK_WIDTH,), jnp.float32) ** block_levels(key_of[9], (QK_WIDTH,), ((0, 16),), -0.2, 0.2)), 0.5, 2.0),
        "key_scale": jnp.clip(jnp.exp(math.log(2.0) - 1.3862944 * jax.random.uniform(key_of[10], (QK_WIDTH,), jnp.float32) ** block_levels(key_of[10], (QK_WIDTH,), ((0, 16),), -0.2, 0.2)), 0.5, 2.0),
        "value_scale": jnp.clip(jnp.exp(math.log(2.0) - 1.3862944 * jax.random.uniform(key_of[11], (V_WIDTH,), jnp.float32) ** block_levels(key_of[11], (V_WIDTH,), ((0, 16),), -0.2, 0.2)), 0.5, 2.0),
        "out_scale": jnp.clip(jnp.exp(math.log(2.0) - 1.3862944 * jax.random.uniform(key_of[12], (D,), jnp.float32) ** block_levels(key_of[12], (D,), ((0, 4),), -0.2, 0.2)), 0.5, 2.0),
        "gate_scale": jnp.clip(jnp.exp(math.log(2.0) - 1.3862944 * jax.random.uniform(key_of[13], (FF,), jnp.float32) ** block_levels(key_of[13], (FF,), ((0, 16),), -0.2, 0.2)), 0.5, 2.0),
        "up_scale": jnp.clip(jnp.exp(math.log(2.0) - 1.3862944 * jax.random.uniform(key_of[14], (FF,), jnp.float32) ** block_levels(key_of[14], (FF,), ((0, 16),), -0.2, 0.2)), 0.5, 2.0),
        "down_scale": jnp.clip(jnp.exp(math.log(2.0) - 1.3862944 * jax.random.uniform(key_of[15], (D,), jnp.float32) ** block_levels(key_of[15], (D,), ((0, 4),), -0.2, 0.2)), 0.5, 2.0),
        "conv_weight": normal_values(key_of[16], (KERNEL, FF), KERNEL ** -0.5, 3.5, ((1, 4),), jnp.float32),
        "conv_bias": normal_values(key_of[17], (FF,), 0.5, 3.0, ((0, 4),), jnp.float32),
        "first_gain": jnp.clip(1.0 + 0.18 * jax.random.normal(key_of[18], (D,), jnp.float32), 0.1, 1.9),
        "first_bias": normal_values(key_of[19], (D,), 0.5, 3.0, (), jnp.float32),
        "second_gain": jnp.clip(1.0 + 0.18 * jax.random.normal(key_of[20], (D,), jnp.float32), 0.1, 1.9),
        "second_bias": normal_values(key_of[21], (D,), 0.5, 3.0, (), jnp.float32),
    }


norm_eps = 1e-05
residual_gain = 2.0 ** 0.25
angle_base = 10000.0

def rotate_pairs(inputs):
    length, head_count, head_width = inputs.shape
    spike_positions = jnp.arange(length, dtype=jnp.float32)
    frequency = 1.0 / angle_base ** jnp.linspace(0.0, 1.0, head_width // 2, dtype=jnp.float32)
    angles = spike_positions[:, None] * frequency[None, :]
    cosine = jnp.cos(angles)[:, None, :]
    sine_part = jnp.sin(angles)[:, None, :]
    paired = inputs.reshape(length, head_count, head_width // 2, 2)
    even_part = paired[..., 0]
    odd_part = paired[..., 1]
    turned = jnp.stack([even_part * cosine - odd_part * sine_part, odd_part * cosine + even_part * sine_part], -1)
    return turned.reshape(inputs.shape)

def retain(queries, key_rows, values, decay_logs):
    length, head_count, key_width = queries.shape
    value_width = values.shape[2]
    blocks = length // BLOCK
    highest = lax.Precision.HIGHEST
    query_blocks = queries.reshape(blocks, BLOCK, head_count, key_width).astype(jnp.float32)
    key_blocks = key_rows.reshape(blocks, BLOCK, head_count, key_width).astype(jnp.float32)
    value_blocks = values.reshape(blocks, BLOCK, head_count, value_width).astype(jnp.float32)
    cumulative = jnp.cumsum(decay_logs.reshape(head_count, blocks, BLOCK), axis=2)
    offsets = jnp.arange(BLOCK)
    causal = offsets[:, None] >= offsets[None, :]
    distance = cumulative[:, :, :, None] - cumulative[:, :, None, :]
    damping = jnp.where(causal, jnp.exp(jnp.where(causal, distance, 0.0)), 0.0)
    scores = jnp.einsum('nqhd,nkhd->hnqk', query_blocks, key_blocks, precision=highest)
    weighted = lax.optimization_barrier((scores * damping).astype(jnp.bfloat16)).astype(jnp.float32)
    within = jnp.einsum('hnqk,nkhv->nqhv', weighted, value_blocks, precision=highest)
    to_end = jnp.exp(cumulative[:, :, -1:] - cumulative)
    from_start = jnp.exp(cumulative)
    carried = jnp.zeros((head_count, key_width, value_width), jnp.float32)
    carried_parts = []
    for segment in range(blocks):
        query_decayed = query_blocks[segment] * from_start[:, segment, :].T[:, :, None]
        carried_parts.append(jnp.einsum('qhd,hdv->qhv', query_decayed, carried, precision=highest))
        key_decayed = key_blocks[segment] * to_end[:, segment, :].T[:, :, None]
        update = jnp.einsum('khd,khv->hdv', key_decayed, value_blocks[segment], precision=highest)
        carried = from_start[:, segment, -1][:, None, None] * carried + update
    return (within + jnp.stack(carried_parts)).reshape(length, head_count, value_width)

def head_norm(outputs):
    centred = outputs - lax.optimization_barrier(jnp.mean(outputs, -1, keepdims=True))
    variance = lax.optimization_barrier(jnp.mean(centred * centred, -1, keepdims=True))
    return centred * lax.rsqrt(variance + norm_eps)

def layer_norm(inputs, gain_vector, offset):
    centred = inputs - lax.optimization_barrier(jnp.mean(inputs, -1, keepdims=True))
    variance = lax.optimization_barrier(jnp.mean(centred * centred, -1, keepdims=True))
    return centred * lax.rsqrt(variance + norm_eps) * gain_vector + offset

def partial_rounded(inputs, weight):
    groups = inputs.reshape(inputs.shape[0], N_TP, -1).astype(jnp.float32)
    stacked = weight.reshape(N_TP, -1, weight.shape[1]).astype(jnp.float32)
    partial_value = jnp.einsum('sgc,gcd->gsd', groups, stacked, precision=lax.Precision.HIGHEST)
    rounded = lax.optimization_barrier(partial_value.astype(jnp.bfloat16)).astype(jnp.float32)
    return lax.optimization_barrier(jnp.sum(rounded, axis=0))

def one_sequence(tokens, decay_logs, query_half, key_half, value_half, out_half, gate_half, up_half, down_half, query_scale, key_scale, value_scale, out_scale, gate_scale, up_scale, down_scale, conv_weight, conv_bias, first_gain, first_bias, second_gain, second_bias):
    length = tokens.shape[0]
    query_raw = jnp.dot(tokens, query_half, preferred_element_type=jnp.float32)
    key_raw = jnp.dot(tokens, key_half, preferred_element_type=jnp.float32)
    value_raw = jnp.dot(tokens, value_half, preferred_element_type=jnp.float32)
    queries = rotate_pairs((query_raw * query_scale).reshape(length, RETENTION_HEADS, QK_HEAD)).astype(jnp.bfloat16)
    key_rows = (rotate_pairs((key_raw * key_scale).reshape(length, RETENTION_HEADS, QK_HEAD)) * QK_HEAD ** (-0.5)).astype(jnp.bfloat16)
    values = (value_raw * value_scale).astype(jnp.bfloat16).reshape(length, RETENTION_HEADS, V_HEAD)
    retained = retain(queries, key_rows, values, decay_logs)
    normed = head_norm(retained).astype(jnp.bfloat16).reshape(length, RETENTION_HEADS * V_HEAD)
    branch = partial_rounded(normed, out_half) * out_scale
    first = layer_norm(residual_gain * tokens.astype(jnp.float32) + branch, first_gain, first_bias).astype(jnp.bfloat16)
    gate = jnp.dot(first, gate_half, preferred_element_type=jnp.float32) * gate_scale
    up_part = jnp.dot(first, up_half, preferred_element_type=jnp.float32) * up_scale
    padded = jnp.pad(gate, ((KERNEL - 1, 0), (0, 0)))
    convolved = conv_bias + jnp.zeros_like(gate)
    for tap_index in range(KERNEL):
        convolved = convolved + padded[tap_index:tap_index + length] * conv_weight[tap_index]
    activated = (jax.nn.gelu(convolved, approximate=False) * up_part).astype(jnp.bfloat16)
    feed = partial_rounded(activated, down_half) * down_scale
    return layer_norm(residual_gain * first.astype(jnp.float32) + feed, second_gain, second_bias).astype(jnp.bfloat16)

def reference(tokens, decay_logs, query_weight, key_weight, value_weight, out_weight, gate_weight, up_weight, down_weight, query_scale, key_scale, value_scale, out_scale, gate_scale, up_scale, down_scale, conv_weight, conv_bias, first_gain, first_bias, second_gain, second_bias):
    sequence_list = tokens.shape[0] // SEQUENCE_TOKENS
    token_seqs = tokens.reshape(sequence_list, SEQUENCE_TOKENS, D)
    decay_seqs = decay_logs.reshape(RETENTION_HEADS, sequence_list, SEQUENCE_TOKENS).transpose(1, 0, 2)
    query_half = query_weight.astype(jnp.bfloat16)
    key_half = key_weight.astype(jnp.bfloat16)
    value_half = value_weight.astype(jnp.bfloat16)
    out_half = out_weight.astype(jnp.bfloat16)
    gate_half = gate_weight.astype(jnp.bfloat16)
    up_half = up_weight.astype(jnp.bfloat16)
    down_half = down_weight.astype(jnp.bfloat16)

    def run_one(paired):
        return one_sequence(paired[0], paired[1], query_half, key_half, value_half, out_half, gate_half, up_half, down_half, query_scale, key_scale, value_scale, out_scale, gate_scale, up_scale, down_scale, conv_weight, conv_bias, first_gain, first_bias, second_gain, second_bias)
    outputs = lax.map(run_one, (token_seqs, decay_seqs))
    return outputs.reshape(sequence_list * SEQUENCE_TOKENS, D)
```

```python
import functools

import jax
import jax.numpy as jnp
import numpy as np
from jax import lax
from jax.experimental import pallas as pl
from jax.experimental.pallas import tpu as pltpu
from jax.sharding import PartitionSpec as P

QK_HEAD = 128
V_HEAD = 256
BLOCK = 128
KERNEL = 3


norm_eps = 1e-05
residual_gain = 2.0**0.25
angle_base = 10000.0


def rotate_pairs(inputs):
    length, head_count, head_width = inputs.shape
    spike_positions = jnp.arange(length, dtype=jnp.float32)
    frequency = 1.0 / angle_base ** jnp.linspace(0.0, 1.0, head_width // 2, dtype=jnp.float32)
    angles = spike_positions[:, None] * frequency[None, :]
    cosine = jnp.cos(angles)[:, None, :]
    sine_part = jnp.sin(angles)[:, None, :]
    paired = inputs.reshape(length, head_count, head_width // 2, 2)
    even_part = paired[..., 0]
    odd_part = paired[..., 1]
    turned = jnp.stack(
        [even_part * cosine - odd_part * sine_part, odd_part * cosine + even_part * sine_part], -1
    )
    return turned.reshape(inputs.shape)


def retain(queries, key_rows, values, decay_logs):
    length, head_count, key_width = queries.shape
    value_width = values.shape[2]
    blocks = length // BLOCK
    highest = lax.Precision.HIGHEST
    query_blocks = queries.reshape(blocks, BLOCK, head_count, key_width).astype(jnp.float32)
    key_blocks = key_rows.reshape(blocks, BLOCK, head_count, key_width).astype(jnp.float32)
    value_blocks = values.reshape(blocks, BLOCK, head_count, value_width).astype(jnp.float32)
    cumulative = jnp.cumsum(decay_logs.reshape(head_count, blocks, BLOCK), axis=2)
    offsets = jnp.arange(BLOCK)
    causal = offsets[:, None] >= offsets[None, :]
    distance = cumulative[:, :, :, None] - cumulative[:, :, None, :]
    damping = jnp.where(causal, jnp.exp(jnp.where(causal, distance, 0.0)), 0.0)
    scores = jnp.einsum("nqhd,nkhd->hnqk", query_blocks, key_blocks, precision=highest)
    weighted = lax.optimization_barrier((scores * damping).astype(jnp.bfloat16)).astype(jnp.float32)
    within = jnp.einsum("hnqk,nkhv->nqhv", weighted, value_blocks, precision=highest)
    to_end = jnp.exp(cumulative[:, :, -1:] - cumulative)
    from_start = jnp.exp(cumulative)
    carried = jnp.zeros((head_count, key_width, value_width), jnp.float32)
    carried_parts = []
    for segment in range(blocks):
        query_decayed = query_blocks[segment] * from_start[:, segment, :].T[:, :, None]
        carried_parts.append(jnp.einsum("qhd,hdv->qhv", query_decayed, carried, precision=highest))
        key_decayed = key_blocks[segment] * to_end[:, segment, :].T[:, :, None]
        update = jnp.einsum("khd,khv->hdv", key_decayed, value_blocks[segment], precision=highest)
        carried = from_start[:, segment, -1][:, None, None] * carried + update
    return (within + jnp.stack(carried_parts)).reshape(length, head_count, value_width)


def head_norm(outputs):
    centred = outputs - jnp.mean(outputs, -1, keepdims=True)
    variance = jnp.mean(centred * centred, -1, keepdims=True)
    return centred * lax.rsqrt(variance + norm_eps)


def layer_norm(inputs, gain_vector, offset):
    centred = inputs - jnp.mean(inputs, -1, keepdims=True)
    variance = jnp.mean(centred * centred, -1, keepdims=True)
    return centred * lax.rsqrt(variance + norm_eps) * gain_vector + offset


def local(
    tokens,
    decay_logs,
    query_weight,
    key_weight,
    value_weight,
    out_weight,
    gate_weight,
    up_weight,
    down_weight,
    query_scale,
    key_scale,
    value_scale,
    out_scale,
    gate_scale,
    up_scale,
    down_scale,
    conv_weight,
    conv_bias,
    first_gain,
    first_bias,
    second_gain,
    second_bias,
):
    length = tokens.shape[0]
    share = length // lax.axis_size("tp")
    scales = (query_scale, key_scale, value_scale, out_scale, down_scale, gate_scale, up_scale)
    packed = lax.all_gather(jnp.concatenate(scales), "fs", axis=0, tiled=False)
    factors = []
    position = 0
    for scale in scales:
        width = scale.shape[0]
        factors.append(packed[:, position : position + width].reshape(-1))
        position += width
    query_factor, key_factor, value_factor, out_factor, down_factor, gate_factor, up_factor = factors

    def own_part(weight, axis):
        size = weight.shape[axis] // lax.axis_size("grp")
        part = lax.dynamic_slice_in_dim(weight, lax.axis_index("grp") * size, size, axis)
        return part.astype(jnp.bfloat16)

    def gather(part, axis):
        return lax.all_gather(part, ("fs", "grp"), axis=axis, tiled=True)

    qkv_part = jnp.concatenate(
        [own_part(query_weight, 0), own_part(key_weight, 0), own_part(value_weight, 0)], 1
    )
    qkv_full = gather(qkv_part, 0)
    query_width, key_width = query_weight.shape[1], key_weight.shape[1]
    gate_half = gate_weight.astype(jnp.bfloat16)
    up_half = up_weight.astype(jnp.bfloat16)
    down_half = down_weight.astype(jnp.bfloat16)
    groups = lax.axis_size("fs")
    own = lax.axis_index("fs")

    def trade(blocks):
        taken = [lax.dynamic_index_in_dim(blocks, own, 0, keepdims=False)]
        for step in range(1, groups):
            block = lax.dynamic_index_in_dim(blocks, (own + step) % groups, 0, keepdims=False)
            ring = [(at, (at + step) % groups) for at in range(groups)]
            taken.append(lax.ppermute(block, "fs", ring))
        return taken

    def trade_all(shard):
        taken = [shard]
        for step in range(1, groups):
            ring = [(at, (at + step) % groups) for at in range(groups)]
            taken.append(lax.ppermute(shard, "fs", ring))
        return taken

    def column_blocks(weight):
        rows, columns = weight.shape
        return weight.reshape(rows, groups, columns // groups).transpose(1, 0, 2)

    units = gate_scale.shape[0]
    move_rows = 2 * groups * length <= 3 * gate_weight.shape[1]
    if move_rows:
        pair = jnp.concatenate([column_blocks(gate_half), column_blocks(up_half)], 2)
        qkv_full, pair, down_half = lax.optimization_barrier((qkv_full, pair, down_half))
    query_full = qkv_full[:, :query_width]
    key_full = qkv_full[:, query_width : query_width + key_width]
    value_full = qkv_full[:, query_width + key_width :]
    if move_rows:
        pair_parts = trade(pair)
        down_parts = trade(down_half.reshape(groups, units, down_half.shape[1]))
    query_raw = jnp.dot(tokens, query_full, preferred_element_type=jnp.float32)
    key_raw = jnp.dot(tokens, key_full, preferred_element_type=jnp.float32)
    value_raw = jnp.dot(tokens, value_full, preferred_element_type=jnp.float32)
    head_count = query_raw.shape[1] // QK_HEAD
    queries = rotate_pairs((query_raw * query_factor).reshape(length, head_count, QK_HEAD)).astype(
        jnp.bfloat16
    )
    key_rows = (
        rotate_pairs((key_raw * key_factor).reshape(length, head_count, QK_HEAD))
        * QK_HEAD ** (-0.5)
    ).astype(jnp.bfloat16)
    values = (value_raw * value_factor).astype(jnp.bfloat16).reshape(length, head_count, V_HEAD)
    retained = retain(queries, key_rows, values, decay_logs)
    normed = head_norm(retained).astype(jnp.bfloat16).reshape(length, head_count * V_HEAD)
    out_full = gather(own_part(out_weight, 1), 1)

    def spread(rows, parts):
        width = parts[0].shape[1]
        filled = jnp.zeros((rows.shape[0], groups * width), jnp.bfloat16)
        for step in range(groups):
            start = (own + groups - step) % groups * width
            product = jnp.dot(rows, parts[step], preferred_element_type=jnp.float32)
            filled = lax.dynamic_update_slice_in_dim(filled, product.astype(jnp.bfloat16), start, 1)
        return filled

    branch = (
        lax.psum_scatter(jnp.dot(normed, out_full, preferred_element_type=jnp.float32).astype(jnp.bfloat16), "tp", scatter_dimension=0, tiled=True).astype(
            jnp.float32
        )
        * out_factor
    )
    own_rows = lax.dynamic_slice_in_dim(tokens, lax.axis_index("tp") * share, share, 0)
    first = layer_norm(
        residual_gain * own_rows.astype(jnp.float32) + branch, first_gain, first_bias
    ).astype(jnp.bfloat16)
    if not move_rows:
        first_all = lax.all_gather(first, "tp", axis=0, tiled=True)
        gate_full = gather(own_part(gate_weight, 0), 0)
        up_full = gather(own_part(up_weight, 0), 0)
        gate_raw = jnp.dot(first_all, gate_full, preferred_element_type=jnp.float32)
        up_raw = jnp.dot(first_all, up_full, preferred_element_type=jnp.float32)
        gate = gate_raw * gate_factor
        up_part = up_raw * up_factor
        padded = jnp.pad(gate, ((KERNEL - 1, 0), (0, 0)))
        convolved = conv_bias + jnp.zeros_like(gate)
        for tap_index in range(KERNEL):
            convolved = convolved + padded[tap_index : tap_index + length] * conv_weight[tap_index]
        activated = (jax.nn.gelu(convolved, approximate=False) * up_part).astype(jnp.bfloat16)
        down_full = gather(own_part(down_weight, 1), 1)
        picked = activated
        feed = (
            lax.psum_scatter(
                jnp.dot(picked, down_full, preferred_element_type=jnp.float32).astype(jnp.bfloat16),
                "tp",
                scatter_dimension=0,
                tiled=True,
            ).astype(jnp.float32)
            * down_factor
        )
        return layer_norm(
            residual_gain * first.astype(jnp.float32) + feed, second_gain, second_bias
        ).astype(jnp.bfloat16)
    first, pair_parts = lax.optimization_barrier((first, pair_parts))
    first_rows = jnp.stack(trade_all(first))
    first_all = lax.all_gather(first_rows, "tp", axis=1, tiled=True).reshape(groups * length, -1)
    depth = gate_weight.shape[0]
    total = 0.0
    for step in range(groups):
        start = (own + groups - step) % groups * depth
        chunk = lax.dynamic_slice_in_dim(first_all, start, depth, 1)
        total = total + jnp.dot(chunk, pair_parts[step], preferred_element_type=jnp.float32)
    gate = (total[:, :units] * gate_scale).reshape(groups, length, units)
    up_part = (total[:, units:] * up_scale).reshape(groups, length, units)
    own_taps = lax.dynamic_slice_in_dim(conv_weight, own * units, units, 1)
    own_bias = lax.dynamic_slice_in_dim(conv_bias, own * units, units, 0)
    padded = jnp.pad(gate, ((0, 0), (KERNEL - 1, 0), (0, 0)))
    convolved = own_bias + jnp.zeros_like(gate)
    for tap_index in range(KERNEL):
        convolved = convolved + padded[:, tap_index : tap_index + length] * own_taps[tap_index]
    activated = (jax.nn.gelu(convolved, approximate=False) * up_part).astype(jnp.bfloat16)
    activated = activated.reshape(groups * length, units)
    shares = spread(activated, down_parts).reshape(groups, length, -1)
    summed = lax.psum_scatter(shares, "tp", scatter_dimension=1, tiled=True)
    feed = summed[0].astype(jnp.float32)
    for step in range(1, groups):
        pairs = [(at, (at + groups - step) % groups) for at in range(groups)]
        feed = feed + lax.ppermute(summed[step], "fs", pairs).astype(jnp.float32)
    feed = feed * down_factor
    return layer_norm(
        residual_gain * first.astype(jnp.float32) + feed, second_gain, second_bias
    ).astype(jnp.bfloat16)


MESH_ID = pl.DeviceIdType.MESH
LANES = 128
QKV_CHUNKS = 2
OUT_CHUNKS = 1
SENDS = 160


def fused_fits(mesh):
    return mesh.shape["fs"] == 4 and mesh.shape["tp"] == 4 and mesh.shape["grp"] == 2


def layer_kernel(
    tokens_hbm,
    query_hbm,
    key_hbm,
    value_hbm,
    out_hbm,
    gate_hbm,
    up_hbm,
    down_hbm,
    small_ref,
    units_ref,
    norm_ref,
    cosine_ref,
    sine_ref,
    result_ref,
    tokens,
    query_f32,
    key_f32,
    value_f32,
    out_f32,
    gate_f32,
    up_f32,
    down_f32,
    qkv_w,
    out_w,
    pair_own,
    pair_w,
    down_own,
    down_w,
    scales,
    out_scale,
    down_scale,
    qkv_raw,
    normed,
    shares,
    shares_in,
    rows,
    first_f32,
    total,
    activated,
    feed,
    feed_core,
    feed_x,
    feed_z,
    load_sem,
    send_sem,
    scale_sem,
    qkv_z,
    qkv_y,
    out_z,
    out_y,
    pair_z,
    pair_y,
    down_z,
    down_y,
    share_sem,
    rows_z,
    rows_x,
    rows_core,
    feed_core_sem,
    feed_x_sem,
    feed_z_sem,
):
    g, f, t = lax.axis_index("grp"), lax.axis_index("fs"), lax.axis_index("tp")
    groups = 4
    beside = f + 1 - 2 * (f % 2)
    near = 2 - f // 2
    far = 3 * (1 - f // 2)
    is_mid = (f + 1) // 2 == 1
    twin = {"grp": 1 - g}
    core, across, corner = t + 1 - 2 * (t % 2), (t + 2) % 4, 3 - t
    parity, side = t % 2, t // 2

    length, width = tokens.shape
    depth = query_f32.shape[0]
    half_depth = depth // 2
    query_width, value_width = query_f32.shape[1], value_f32.shape[1]
    qkv_width = qkv_w.shape[1]
    out_columns = out_f32.shape[1]
    units = down_own.shape[1]
    padded_units = activated.shape[1]
    share = length // groups
    own_columns = gate_f32.shape[1]

    pending = []

    def send(src, dst, arrival, device, when=None):
        index = len(pending)
        copy = pltpu.make_async_remote_copy(
            src_ref=src, dst_ref=dst, send_sem=send_sem.at[index], recv_sem=arrival, device_id=device, device_id_type=MESH_ID
        )
        if when is None:
            copy.start()
        else:
            pl.when(when)(copy.start)
        pending.append((copy, when))

    def arrived(ref, arrival):
        pltpu.make_async_remote_copy(
            src_ref=ref, dst_ref=ref, send_sem=send_sem.at[SENDS - 1], recv_sem=arrival, device_id=twin, device_id_type=MESH_ID
        ).wait_recv()

    def tiles(count, body):
        lax.fori_loop(0, count, lambda i, c: (body(i), c)[1], 0)

    barrier = pltpu.get_barrier_semaphore()
    for partner in ({"fs": beside}, {"fs": near}, {"fs": far}, twin, {"tp": core}, {"tp": across}, {"tp": corner}):
        pl.semaphore_signal(barrier, inc=1, device_id=partner, device_id_type=MESH_ID)
    pairs = (
        (query_hbm, query_f32),
        (key_hbm, key_f32),
        (value_hbm, value_f32),
        (out_hbm, out_f32),
        (tokens_hbm, tokens),
        (gate_hbm, gate_f32),
        (up_hbm, up_f32),
        (down_hbm, down_f32),
    )
    loads = [pltpu.make_async_copy(a, b, load_sem.at[i]) for i, (a, b) in enumerate(pairs)]
    for load in loads:
        load.start()
    for load in loads[:3]:
        load.wait()

    chunk_rows = 64
    own_start = f * depth

    def cast_qkv(i):
        at = pl.ds(pl.multiple_of(i * chunk_rows, chunk_rows), chunk_rows)
        to = pl.ds(pl.multiple_of(own_start + i * chunk_rows, chunk_rows), chunk_rows)
        qkv_w[to, 0:query_width] = query_f32[at, :].astype(jnp.bfloat16)
        qkv_w[to, query_width : 2 * query_width] = key_f32[at, :].astype(jnp.bfloat16)
        qkv_w[to, 2 * query_width : qkv_width] = value_f32[at, :].astype(jnp.bfloat16)

    tiles(depth // chunk_rows, cast_qkv)
    scales[f] = small_ref[...]
    pl.semaphore_wait(barrier, 7)


    for other in (beside, near, far):
        send(small_ref, scales.at[f], scale_sem.at[f], {"fs": other})

    def qkv_piece(src, half, chunk):
        size = half_depth // QKV_CHUNKS
        start = src * depth + half * half_depth + chunk * size
        return qkv_w.at[pl.ds(pl.multiple_of(start, size), size)]

    def out_piece(src, half, chunk):
        size = out_w.shape[1] // 2 // OUT_CHUNKS
        start = half * (out_w.shape[1] // 2) + chunk * size
        return out_w.at[src, pl.ds(pl.multiple_of(start, size), size)]

    for other in (beside, near):
        for chunk in range(QKV_CHUNKS):
            piece = qkv_piece(f, g, chunk)
            send(piece, piece, qkv_z.at[f, chunk], {"fs": other})

    loads[3].wait()
    tiles(
        out_f32.shape[0] // chunk_rows,
        lambda i: out_w.__setitem__(
            (f, pl.ds(pl.multiple_of(i * chunk_rows, chunk_rows), chunk_rows)),
            out_f32[pl.ds(pl.multiple_of(i * chunk_rows, chunk_rows), chunk_rows), :].astype(jnp.bfloat16),
        ),
    )
    for chunk in range(OUT_CHUNKS):
        piece = out_piece(f, g, chunk)
        send(piece, piece, out_z.at[f, chunk], {"fs": near})
    for load in loads[4:]:
        load.wait()
    cast_rows = 32

    def cast_pair(i):
        at = pl.ds(pl.multiple_of(i * cast_rows, cast_rows), cast_rows)
        for ref, base in ((gate_f32, 0), (up_f32, padded_units)):
            values = ref[at, :]
            for block in range(groups):
                turned = values if block == 0 else pltpu.roll(values, own_columns - block * units, 1)
                pair_own[block, at, base : base + padded_units] = turned[:, :padded_units].astype(jnp.bfloat16)

    tiles(depth // cast_rows, cast_pair)
    for block in range(groups):
        down_own[block] = down_f32[block * units : (block + 1) * units, :].astype(jnp.bfloat16)
    pair_w[pl.ds(pl.multiple_of(own_start, depth), depth), :] = pair_own[f]
    for block in range(groups):
        down_w[block, units:padded_units, :] = jnp.zeros((padded_units - units, out_columns), jnp.bfloat16)
    down_w[f, 0:units, :] = down_own[f]

    for src in (beside, near, far):
        for chunk in range(QKV_CHUNKS):
            piece = qkv_piece(src, g, chunk)
            arrived(piece, qkv_z.at[src, chunk])
            send(piece, piece, qkv_y.at[src, chunk], twin)
            if src is not beside:
                send(piece, piece, qkv_z.at[src, chunk], {"fs": beside}, is_mid)
    for chunk in range(OUT_CHUNKS):
        piece = out_piece(f, g, chunk)
        send(piece, piece, out_z.at[f, chunk], {"fs": beside})

    def pair_piece(ref, src, half):
        return ref.at[pl.ds(pl.multiple_of(src * depth + half * half_depth, half_depth), half_depth)]

    for other in (near, far, beside):
        own = pair_own.at[other, pl.ds(pl.multiple_of(g * half_depth, half_depth), half_depth)]
        send(own, pair_piece(pair_w, f, g), pair_z.at[f], {"fs": other})
    for src in (near, far):

        @pl.when(is_mid)
        def _():
            for chunk in range(OUT_CHUNKS):
                arrived(out_piece(src, g, chunk), out_z.at[src, chunk])

        for chunk in range(OUT_CHUNKS):
            piece = out_piece(src, g, chunk)
            send(piece, piece, out_z.at[src, chunk], {"fs": beside}, is_mid)
            send(piece, piece, out_y.at[src, chunk], twin, is_mid)

    column_tile = 512

    def add_product(src, first):
        start = pl.multiple_of(src * depth, depth)

        def body(i):
            at = pl.ds(pl.multiple_of(i * column_tile, column_tile), column_tile)
            product = jnp.dot(
                tokens[:, pl.ds(start, depth)], qkv_w[pl.ds(start, depth), at], preferred_element_type=jnp.float32
            )
            if first:
                qkv_raw[:, at] = product
            else:
                qkv_raw[:, at] += product

        tiles(qkv_width // column_tile, body)

    add_product(f, True)
    for src in (beside, near, far):
        arrived(scales.at[src], scale_sem.at[src])
    for src in (beside, near, far):
        for chunk in range(QKV_CHUNKS):
            arrived(qkv_piece(src, 1 - g, chunk), qkv_y.at[src, chunk])
        add_product(src, False)

    merged = scales[0] + scales[1] + scales[2] + scales[3]
    query_scale = merged[2:3, 0:query_width]
    key_scale = merged[2:3, query_width : 2 * query_width]
    value_scale = merged[3:4, 0:value_width]
    for src in range(groups):
        out_scale[:, src * out_columns : (src + 1) * out_columns] = scales[src, 0:1, :]
        down_scale[:, src * out_columns : (src + 1) * out_columns] = scales[src, 1:2, :]

    row_at = lax.broadcasted_iota(jnp.int32, (length, length), 0)
    column_at = lax.broadcasted_iota(jnp.int32, (length, length), 1)
    causal = row_at >= column_at
    triangle = causal.astype(jnp.float32)
    decay = small_ref[:, 0:length]
    summed_columns = lax.dot_general(
        triangle, decay, (((1,), (1,)), ((), ())), precision=lax.Precision.HIGHEST, preferred_element_type=jnp.float32
    )
    summed_rows = lax.dot_general(
        decay, triangle, (((1,), (1,)), ((), ())), precision=lax.Precision.HIGHEST, preferred_element_type=jnp.float32
    )
    even = lax.broadcasted_iota(jnp.int32, (length, QK_HEAD), 1) % 2 == 0

    def rotate(values):
        swapped = jnp.where(even, pltpu.roll(values, QK_HEAD - 1, 1), pltpu.roll(values, 1, 1))
        return values * cosine_ref[...] + swapped * sine_ref[...]

    for head in range(query_width // QK_HEAD):
        at = slice(head * QK_HEAD, (head + 1) * QK_HEAD)
        key_at = slice(query_width + head * QK_HEAD, query_width + (head + 1) * QK_HEAD)
        wide = slice(head * V_HEAD, (head + 1) * V_HEAD)
        value_at = slice(2 * query_width + head * V_HEAD, 2 * query_width + (head + 1) * V_HEAD)
        queries = rotate(qkv_raw[:, at] * query_scale[:, at]).astype(jnp.bfloat16)
        key_rows = (rotate(qkv_raw[:, key_at] * key_scale[:, at]) * QK_HEAD ** (-0.5)).astype(jnp.bfloat16)
        values = (qkv_raw[:, value_at] * value_scale[:, wide]).astype(jnp.bfloat16)
        scores = lax.dot_general(queries, key_rows, (((1,), (1,)), ((), ())), preferred_element_type=jnp.float32)
        distance = summed_columns[:, 4 + head : 5 + head] - summed_rows[4 + head : 5 + head, :]
        damping = jnp.where(causal, jnp.exp(jnp.where(causal, distance, 0.0)), 0.0)
        weighted = (scores * damping).astype(jnp.bfloat16)
        retained = jnp.dot(weighted, values, preferred_element_type=jnp.float32)
        centred = retained - jnp.mean(retained, -1, keepdims=True)
        variance = jnp.mean(centred * centred, -1, keepdims=True)
        normed[:, wide] = (centred * lax.rsqrt(variance + norm_eps)).astype(jnp.bfloat16)

    for src in (beside, near, far):
        late = None if src is beside else jnp.logical_not(is_mid)

        def wait_out(src=src):
            for chunk in range(OUT_CHUNKS):
                arrived(out_piece(src, g, chunk), out_z.at[src, chunk])

        if late is None:
            wait_out()
        else:
            pl.when(late)(wait_out)
        for chunk in range(OUT_CHUNKS):
            piece = out_piece(src, g, chunk)
            send(piece, piece, out_y.at[src, chunk], twin, late)

    def out_product(src):
        product = jnp.dot(normed[...], out_w[src], preferred_element_type=jnp.float32).astype(jnp.bfloat16)
        at = pl.ds(pl.multiple_of(src * out_columns, out_columns), out_columns)
        for block in range(groups):
            shares[block, :, at] = product[block * share : (block + 1) * share, :]

    out_product(f)
    for src in (beside, near, far):
        for chunk in range(OUT_CHUNKS):
            arrived(out_piece(src, 1 - g, chunk), out_y.at[src, chunk])
        out_product(src)
    for other in (across, corner, core):
        send(shares.at[other], shares_in.at[t], share_sem.at[t], {"tp": other})

    for src in (beside, near, far):
        piece = pair_piece(pair_w, src, g)
        arrived(piece, pair_z.at[src])
        send(piece, piece, pair_y.at[src], twin)

    branch = shares[t].astype(jnp.float32)
    for other in (core, across, corner):
        arrived(shares_in.at[other], share_sem.at[other])
        branch = branch + shares_in[other].astype(jnp.float32)

    def layer_norm_rows(values, gain, bias):
        centred = values - jnp.mean(values, -1, keepdims=True)
        variance = jnp.mean(centred * centred, -1, keepdims=True)
        return centred * lax.rsqrt(variance + norm_eps) * gain + bias

    own_rows = pl.ds(pl.multiple_of(t * share, share), share)
    mixed = residual_gain * tokens[own_rows, :].astype(jnp.float32) + branch * out_scale[...]
    first = layer_norm_rows(mixed, norm_ref[0:1, :], norm_ref[1:2, :]).astype(jnp.bfloat16)
    first_f32[...] = first.astype(jnp.float32)
    rows[f, own_rows, :] = first

    def block(seq, who):
        return rows.at[seq, pl.ds(pl.multiple_of(who * share, share), share)]

    own = block(f, t)
    send(own, own, rows_z.at[f], {"fs": near})
    send(own, own, rows_z.at[f], {"fs": beside})
    send(own, own, rows_x.at[f], {"tp": across})
    send(own, own, rows_core.at[f, 0], {"tp": core})

    half_units = units // 2

    def down_piece(ref, at, half):
        return ref.at[at, pl.ds(pl.multiple_of(half * half_units, half_units), half_units)]

    for other in (near, far, beside):
        send(down_piece(down_own, other, g), down_piece(down_w, f, g), down_z.at[f], {"fs": other})
    for src in (beside, near, far):
        piece = block(src, t)
        arrived(piece, rows_z.at[src])
        if src is not beside:
            send(piece, piece, rows_z.at[src], {"fs": beside}, is_mid)
        send(piece, piece, rows_x.at[src], {"tp": across})
        send(piece, piece, rows_core.at[src, 0], {"tp": core})
    for src in (beside, near, far):
        arrived(pair_piece(pair_w, src, 1 - g), pair_y.at[src])

    gate_scale, up_scale = units_ref[0:1, :], units_ref[1:2, :]
    conv_bias = units_ref[2:3, :]
    row_in = lax.broadcasted_iota(jnp.int32, (length, padded_units), 0)
    wide_tile = 2 * LANES

    def units_of(seq):
        piece = block(seq, across)
        arrived(piece, rows_x.at[seq])
        send(piece, piece, rows_core.at[seq, 1], {"tp": core})
        arrived(block(seq, core), rows_core.at[seq, 0])
        arrived(block(seq, corner), rows_core.at[seq, 1])

        def body(i):
            at = pl.ds(pl.multiple_of(i * wide_tile, wide_tile), wide_tile)
            total[:, at] = jnp.dot(rows[seq], pair_w[:, at], preferred_element_type=jnp.float32)

        tiles(2 * padded_units // wide_tile, body)
        gate = total[:, 0:padded_units] * gate_scale
        convolved = conv_bias + gate * units_ref[2 + KERNEL : 3 + KERNEL, :]
        for back in range(1, KERNEL):
            shifted = jnp.where(row_in >= back, pltpu.roll(gate, back, 0), 0.0)
            convolved = convolved + shifted * units_ref[2 + KERNEL - back : 3 + KERNEL - back, :]
        gelu = 0.5 * convolved * (1.0 + lax.erf(convolved * np.float32(np.sqrt(0.5))))
        activated[...] = (gelu * (total[:, padded_units:] * up_scale)).astype(jnp.bfloat16)

    def feed_of(seq):
        def body(src):
            product = jnp.dot(activated[...], down_w[src], preferred_element_type=jnp.float32).astype(jnp.bfloat16)
            at = pl.ds(pl.multiple_of(src * out_columns, out_columns), out_columns)
            for who in range(groups):
                feed[seq, who % 2, who // 2, :, at] = product[who * share : (who + 1) * share, :]

        tiles(groups, body)
        send(feed.at[seq, 1 - parity], feed_core.at[seq], feed_core_sem.at[seq], {"tp": core})

    def join_cores(seq):
        arrived(feed_core.at[seq], feed_core_sem.at[seq])
        for to in range(2):
            both = feed[seq, parity, to].astype(jnp.float32) + feed_core[seq, to].astype(jnp.float32)
            feed[seq, parity, to] = both.astype(jnp.bfloat16)
        send(feed.at[seq, parity, 1 - side], feed_x.at[seq], feed_x_sem.at[seq], {"tp": across})

    def join_across(seq):
        arrived(feed_x.at[seq], feed_x_sem.at[seq])
        both = feed[seq, parity, side].astype(jnp.float32) + feed_x[seq].astype(jnp.float32)
        feed[seq, parity, side] = both.astype(jnp.bfloat16)
        if seq is not f:
            send(feed.at[seq, parity, side], feed_z.at[f], feed_z_sem.at[f], {"fs": seq})

    order = (f, beside, near, far)
    for at in range(groups + 2):
        if at < groups:
            units_of(order[at])
            if at == 0:
                for src in (beside, near, far):
                    piece = down_piece(down_w, src, g)
                    arrived(piece, down_z.at[src])
                    send(piece, piece, down_y.at[src], twin)
                for src in (beside, near, far):
                    arrived(down_piece(down_w, src, 1 - g), down_y.at[src])
            feed_of(order[at])
        if 1 <= at <= groups:
            join_cores(order[at - 1])
        if at >= 2:
            join_across(order[at - 2])

    summed = feed[f, parity, side].astype(jnp.float32)
    for src in (beside, near, far):
        arrived(feed_z.at[src], feed_z_sem.at[src])
        summed = summed + feed_z[src].astype(jnp.float32)
    mixed = residual_gain * first_f32[...] + summed * down_scale[...]
    result_ref[...] = layer_norm_rows(mixed, norm_ref[2:3, :], norm_ref[3:4, :]).astype(jnp.bfloat16)

    for copy, when in pending:
        if when is None:
            copy.wait_send()
        else:
            pl.when(when)(copy.wait_send)


def rotation_tables(length):
    frequency = 1.0 / angle_base ** np.linspace(0.0, 1.0, QK_HEAD // 2)
    angles = np.arange(length)[:, None] * frequency[None, :].astype(np.float32).astype(np.float64)
    cosine = np.repeat(np.cos(angles), 2, axis=1)
    sine = np.stack([-np.sin(angles), np.sin(angles)], -1).reshape(length, QK_HEAD)
    return cosine.astype(np.float32), sine.astype(np.float32)


def fused(
    tokens,
    decay_logs,
    query_weight,
    key_weight,
    value_weight,
    out_weight,
    gate_weight,
    up_weight,
    down_weight,
    query_scale,
    key_scale,
    value_scale,
    out_scale,
    gate_scale,
    up_scale,
    down_scale,
    conv_weight,
    conv_bias,
    first_gain,
    first_bias,
    second_gain,
    second_bias,
):
    groups = lax.axis_size("fs")
    own = lax.axis_index("fs")
    length, width = tokens.shape
    depth, query_width = query_weight.shape
    value_width = value_weight.shape[1]
    out_depth, out_columns = out_weight.shape
    units = gate_scale.shape[0]
    own_columns = gate_weight.shape[1]
    padded_units = -(-units // LANES) * LANES
    share = length // lax.axis_size("tp")
    qkv_width = 2 * query_width + value_width
    assert own_columns == groups * units and own_columns % LANES == 0 and out_columns >= max(length, 2 * query_width, value_width)

    def placed(scale, columns):
        return lax.dynamic_update_slice_in_dim(jnp.zeros((columns,), jnp.float32), scale, own * scale.shape[0], 0)

    def row(values):
        return jnp.pad(values, (0, out_columns - values.shape[0]))[None]

    small = jnp.concatenate(
        [
            out_scale[None],
            down_scale[None],
            row(jnp.concatenate([placed(query_scale, query_width), placed(key_scale, query_width)])),
            row(placed(value_scale, value_width)),
            jnp.pad(decay_logs, ((0, 4 - decay_logs.shape[0]), (0, out_columns - length))),
        ]
    )
    taps = lax.dynamic_slice_in_dim(conv_weight, own * units, units, 1)
    bias = lax.dynamic_slice_in_dim(conv_bias, own * units, units, 0)
    per_unit = jnp.concatenate([gate_scale[None], up_scale[None], bias[None], taps])
    per_unit = jnp.pad(per_unit, ((0, 8 - per_unit.shape[0]), (0, padded_units - units)))
    norms = jnp.stack([first_gain, first_bias, second_gain, second_bias])
    cosine, sine = rotation_tables(length)

    half = jnp.bfloat16
    single = jnp.float32
    memory = pltpu.VMEM
    arrivals = pltpu.SemaphoreType.DMA
    anywhere = pl.BlockSpec(memory_space=pl.ANY)
    inside = pl.BlockSpec(memory_space=pltpu.VMEM)
    return pl.pallas_call(
        layer_kernel,
        out_shape=jax.ShapeDtypeStruct((share, width), jnp.bfloat16),
        in_specs=[anywhere] * 8 + [inside] * 5,
        out_specs=inside,
        scratch_shapes=[
            memory(tokens.shape, half),
            memory(query_weight.shape, single),
            memory(key_weight.shape, single),
            memory(value_weight.shape, single),
            memory(out_weight.shape, single),
            memory(gate_weight.shape, single),
            memory(up_weight.shape, single),
            memory(down_weight.shape, single),
            memory((groups * depth, qkv_width), half),
            memory((groups, out_depth, out_columns), half),
            memory((groups, depth, 2 * padded_units), half),
            memory((groups * depth, 2 * padded_units), half),
            memory((groups, units, out_columns), half),
            memory((groups, padded_units, out_columns), half),
            memory((groups, 8, out_columns), single),
            memory((1, width), single),
            memory((1, width), single),
            memory((length, qkv_width), single),
            memory((length, value_width), half),
            memory((groups, share, width), half),
            memory((groups, share, width), half),
            memory((groups, length, width), half),
            memory((share, width), single),
            memory((length, 2 * padded_units), single),
            memory((length, padded_units), half),
            memory((groups, 2, 2, share, width), half),
            memory((groups, 2, share, width), half),
            memory((groups, share, width), half),
            memory((groups, share, width), half),
            arrivals((8,)),
            arrivals((SENDS,)),
            arrivals((groups,)),
            arrivals((groups, QKV_CHUNKS)),
            arrivals((groups, QKV_CHUNKS)),
            arrivals((groups, OUT_CHUNKS)),
            arrivals((groups, OUT_CHUNKS)),
            arrivals((groups,)),
            arrivals((groups,)),
            arrivals((groups,)),
            arrivals((groups,)),
            arrivals((groups,)),
            arrivals((groups,)),
            arrivals((groups,)),
            arrivals((groups, 2)),
            arrivals((groups,)),
            arrivals((groups,)),
            arrivals((groups,)),
        ],
        compiler_params=pltpu.CompilerParams(collective_id=0, has_side_effects=True, vmem_limit_bytes=63 * 2**20),
    )(
        tokens,
        query_weight,
        key_weight,
        value_weight,
        out_weight,
        gate_weight,
        up_weight,
        down_weight,
        small,
        per_unit,
        norms,
        jnp.asarray(cosine),
        jnp.asarray(sine),
    )


def solution(mesh):
    in_specs = (
        P(("grp", "fs"), None),
        P("tp", ("grp", "fs")),
        P("fs", "tp"),
        P("fs", "tp"),
        P("fs", "tp"),
        P("tp", "fs"),
        P("fs", "tp"),
        P("fs", "tp"),
        P("tp", "fs"),
        P(("tp", "fs")),
        P(("tp", "fs")),
        P(("tp", "fs")),
        P("fs"),
        P(("tp", "fs")),
        P(("tp", "fs")),
        P("fs"),
        P(None, "tp"),
        P("tp"),
        P(),
        P(),
        P(),
        P(),
    )
    out_specs = P(("grp", "fs", "tp"), None)
    chosen = fused if fused_fits(mesh) else local
    return jax.shard_map(chosen, mesh=mesh, in_specs=in_specs, out_specs=out_specs, check_vma=False)
```
